32 devices in a mesh: sp: 4 (over y, x), tp: 8 (over z, core).
Axes of the slice: x: 2, y: 2, z: 4, core: 2. Of those that a mesh axis runs over, the one named last changes fastest.
Arguments:
- queries: bfloat16 [3072, 16, 128], P('sp', 'tp'), may hold values from -240 to 240
- key_pairs: bfloat16 [3072, 16, 128], P('sp', 'tp'), may hold values from -11 to 11
- head_values: bfloat16 [3072, 16, 128], P('sp', 'tp'), may hold values from -6 to 6
- lambdas: float32 [16], P('tp'), may hold values from 0.3 to 0.8
- head_gain: float32 [128], replicated, may hold values from 0.1 to 1.9
- out_weight: bfloat16 [2048, 2048], replicated, may hold values from -0.125 to 0.125
- residual: bfloat16 [3072, 2048], P(('sp', 'tp')), may hold values from -6 to 6
- norm_gain: float32 [2048], replicated, may hold values from 0.1 to 1.9
- expert_ids: int32 [3072, 2], P(('sp', 'tp')), may hold values from 0 to 7, all different within a row; in each aligned block of 96 rows (0 to 95, 96 to 191, ...) at most 32 rows name the same one
- route_weights: float32 [3072, 2], P(('sp', 'tp')), may hold values from 0.2 to 1
- gate_weight: bfloat16 [8, 2048, 2048], P('sp', None, 'tp'), may hold values from -0.125 to 0.125
- up_weight: bfloat16 [8, 2048, 2048], P('sp', None, 'tp'), may hold values from -0.125 to 0.125
- down_weight: bfloat16 [8, 2048, 2048], P('sp', 'tp'), may hold values from -0.125 to 0.125
Outputs:
- merged: bfloat16 [3072, 2048], P(('sp', 'tp'))
The draws below stay inside these ranges and needn't reach their ends.
Inputs may be any that keep to these rules, and one draw needn't show every extreme that they name: `expert_ids`: within the rows of one device each expert is named at most 32 times, and exactly 32 times in some device.
All inputs are finite; a program needn't handle non-finite values.
Results may differ from the reference program's by a relative error of at most 0.019.
Values may be sent and summed in bfloat16 or wider, within the bound.
A program may use at most 128 MiB of HBM per device.

```python
import math
import jax
import jax.numpy as jnp
import numpy as np
from jax import lax

D = 2048
HEADS = 16
HD = 64
VD = 128
FF = 2048
TOPK = 2
LENGTH = 3072
ROWS = 96
EXPERTS = 8
CAP = 32
N_TP = 8


def base_field(key, salt_value):
    return jnp.clip(jax.random.normal(jax.random.fold_in(key, salt_value), (LENGTH, HEADS, 2 * HD), jnp.float32), -4.0, 4.0) * 1.3


def draw_key_pairs(key, part):
    drawn_field = base_field(key, 11)
    return drawn_field.astype(jnp.bfloat16)


def draw_queries(key, part):
    drawn_field = base_field(key, 12)
    return drawn_field.astype(jnp.bfloat16)


def block_levels(rng, dims, shards, smallest, largest):
    loudness = 1.0
    for dim, blocks in shards:
        draws = jax.random.uniform(jax.random.fold_in(jax.random.fold_in(rng, 6), dim), (blocks,), jnp.float32, smallest / len(shards), largest / len(shards))
        loudness = loudness * jnp.repeat(jnp.exp(draws), dims[dim] // blocks).reshape((-1,) + (1,) * (len(dims) - 1 - dim))
    return loudness


def shared_out(own_key, own, number, rows, amount, top, limit, lean):
    order = jax.random.permutation(own_key, amount)
    crowded, common = load_shares(amount, rows * top, limit, lean, True), load_shares(amount, rows * top, limit, lean, False)
    places = jnp.arange(amount)

    def named(sizes, rotation):
        used = int((sizes > 0).sum())
        fixed = max(1, used // 4)
        passed = fixed + (places - fixed + rotation * (used - fixed)) % max(1, amount - fixed)
        return jnp.zeros((amount,), jnp.int32).at[order[jnp.where(places < fixed, places, passed)]].set(jnp.asarray(sizes, jnp.int32))

    sizes = jnp.where(number % 4 == 0, named(crowded, number // 4), named(common, number - number // 4 - 1))
    mixed = jax.random.permutation(jax.random.fold_in(own, 3), amount)
    source_of, sink = mixed[0:amount // 2 * 2:2], mixed[1:amount // 2 * 2:2]
    room = jnp.minimum(sizes[source_of] - 1, limit - sizes[sink]) // 2
    room = jnp.where((source_of == order[0]) | (sink == order[0]) | (sizes[sink] == 0), 0, jnp.maximum(room, 0))
    passed = jax.random.randint(jax.random.fold_in(own, 4), (amount // 2,), 0, 1 << 20) % (room + 1)
    sizes = sizes.at[source_of].add(-passed).at[sink].add(passed)
    items = jnp.searchsorted(jnp.cumsum(sizes), jnp.arange(rows * top), side="right").astype(jnp.int32)
    table = items.reshape(top, rows).T
    table = table[jax.random.permutation(jax.random.fold_in(own, 1), rows)]
    rotation = jax.random.randint(jax.random.fold_in(own, 2), (rows, 1), 0, top)
    return jnp.take_along_axis(table, (jnp.arange(top)[None, :] + rotation) % top, axis=1)


def load_shares(count, total, limit, skew, full):
    portions = [(1 << 20) // math.isqrt(grade ** skew) + 1 for grade in range(1, count + 1)]
    largest = limit if full else min(limit, max(-(-total // count), total * portions[0] // sum(portions)))
    least = 1 if total - largest >= count - 1 else 0
    holding, surplus = [largest] + [least] * (count - 1), total - largest - least * (count - 1)
    while surplus > 0:
        free = [i for i in range(1, count) if holding[i] < largest] or [i for i in range(1, count) if holding[i] < limit]
        mass, budget = sum([portions[i] for i in free]), surplus
        for i in free:
            more = min(limit - holding[i], max(1, budget * portions[i] // mass), surplus)
            holding[i] = holding[i] + more
            surplus = surplus - more
    return np.array(holding)


def centred(own_key, extent, scale, most, cuts=(), kind=jnp.bfloat16):
    loudness = block_levels(own_key, extent, cuts, -0.22, 0.18) if cuts else 1.0
    values = jax.random.normal(own_key, extent, jnp.float32) * scale * loudness
    return jnp.minimum(jnp.maximum(values, -most), most).astype(kind)


def setup_inputs(seed: int = 0) -> dict:
    key_list = jax.random.split(jax.random.key(seed), 14)
    queries = draw_queries(jax.random.fold_in(key_list[13], 71), 0)
    key_pairs = draw_key_pairs(jax.random.fold_in(key_list[13], 71), 0)
    head_values = centred(key_list[2], (LENGTH, HEADS, VD), 1.0, 6.0, ((0, 4), (1, 8)))
    lambdas = jnp.clip(0.3 + 0.5 * jax.random.uniform(key_list[3], (HEADS,), jnp.float32) ** block_levels(key_list[3], (HEADS,), ((0, 8),), -0.2, 0.2), 0.3, 0.8)
    head_gain = jnp.clip(1.0 + 0.18 * jax.random.normal(key_list[4], (VD,), jnp.float32), 0.1, 1.9)
    out_weight = centred(key_list[5], (HEADS * VD, D), (HEADS * VD) ** -0.5, 0.125)
    residual = centred(key_list[6], (LENGTH, D), 1.0, 6.0, ((0, 32),))
    norm_gain = jnp.clip(1.0 + 0.18 * jax.random.normal(key_list[7], (D,), jnp.float32), 0.1, 1.9)
    expert_ids_keys = jax.random.split(jax.random.fold_in(key_list[8], 1), LENGTH // ROWS)
    expert_ids_turns = jax.random.permutation(jax.random.fold_in(key_list[8], 3), LENGTH // ROWS)
    expert_ids = jax.vmap(lambda own, number: shared_out(jax.random.fold_in(key_list[8], 2), own, number, ROWS, EXPERTS, TOPK, CAP, 1))(expert_ids_keys, expert_ids_turns).reshape((LENGTH, TOPK))
    route_weights = jnp.clip(0.2 + 0.8 * jax.random.uniform(key_list[9], (LENGTH, TOPK), jnp.float32) ** block_levels(key_list[9], (LENGTH, TOPK), ((0, 32),), -0.2, 0.2), 0.2, 1.0)
    gate_weight = centred(key_list[10], (EXPERTS, D, FF), D ** -0.5, 0.125, ((0, 4), (2, 8)))
    up_weight = centred(key_list[11], (EXPERTS, D, FF), D ** -0.5, 0.125, ((0, 4), (2, 8)))
    down_weight = centred(key_list[12], (EXPERTS, FF, D), FF ** -0.5, 0.125, ((0, 4), (1, 8)))
    return {"queries": queries, "key_pairs": key_pairs, "head_values": head_values, "lambdas": lambdas, "head_gain": head_gain, "out_weight": out_weight, "residual": residual, "norm_gain": norm_gain, "expert_ids": expert_ids, "route_weights": route_weights, "gate_weight": gate_weight, "up_weight": up_weight, "down_weight": down_weight}


def attend_head(query_rows, key_rows, value_rows, weight_two):
    block_rows = min(512, LENGTH)
    columns = jnp.arange(LENGTH, dtype=jnp.int32)

    def one_block(block_index):
        offset = block_index * block_rows
        query_block = lax.dynamic_slice_in_dim(query_rows, offset, block_rows, 0)
        positions = offset + jnp.arange(block_rows, dtype=jnp.int32)
        allowed = columns[None, :] <= positions[:, None]
        results = []
        for member in range(2):
            first_col = member * HD
            scores = jnp.dot(query_block[:, first_col:first_col + HD], key_rows[:, first_col:first_col + HD].T, preferred_element_type=jnp.float32) * HD ** (-0.5)
            scores = jnp.where(allowed, scores, -jnp.inf)
            highest = lax.optimization_barrier(jnp.max(scores, axis=1, keepdims=True))
            weights = jnp.exp(scores - highest)
            totals = lax.optimization_barrier(jnp.sum(weights, axis=1, keepdims=True))
            summed = jnp.dot(weights.astype(jnp.bfloat16), value_rows, preferred_element_type=jnp.float32)
            results.append(summed / totals)
        return results[0] - weight_two * results[1]
    blocks = lax.map(one_block, jnp.arange(LENGTH // block_rows, dtype=jnp.int32))
    return blocks.reshape(LENGTH, VD)

def reference(queries, key_pairs, head_values, lambdas, head_gain, out_weight, residual, norm_gain, expert_ids, route_weights, gate_weight, up_weight, down_weight):

    def one_head(packed):
        query_rows, key_rows, value_rows, weight_two = packed
        mixed = attend_head(query_rows, key_rows, value_rows, weight_two)
        row_scale = lax.rsqrt(lax.optimization_barrier(jnp.mean(mixed * mixed, axis=1, keepdims=True)) + 1e-06)
        return (mixed * row_scale * head_gain).astype(jnp.bfloat16)
    per_head = lax.map(one_head, (jnp.transpose(queries, (1, 0, 2)), jnp.transpose(key_pairs, (1, 0, 2)), jnp.transpose(head_values, (1, 0, 2)), lambdas))
    attended = jnp.transpose(per_head, (1, 0, 2)).reshape(LENGTH, HEADS * VD)
    projected = jnp.dot(attended, out_weight, preferred_element_type=jnp.float32)
    updated = (residual.astype(jnp.float32) + projected).astype(jnp.bfloat16)
    widened = updated.astype(jnp.float32)
    normed = (widened * lax.rsqrt(lax.optimization_barrier(jnp.mean(widened * widened, axis=1, keepdims=True)) + 1e-06) * norm_gain).astype(jnp.bfloat16)
    flat_ids = expert_ids.reshape(-1)
    flat_weights = route_weights.reshape(-1)
    owners = jnp.arange(LENGTH * TOPK, dtype=jnp.int32) // TOPK
    most_rows = LENGTH // ROWS * CAP
    slice_width = FF // N_TP

    def expert_step(gathered, expert):
        matches = flat_ids == expert
        chosen = jnp.nonzero(matches, size=most_rows, fill_value=0)[0].astype(jnp.int32)
        filled = (jnp.arange(most_rows, dtype=jnp.int32) < jnp.sum(matches.astype(jnp.int32))).astype(jnp.float32)
        targets = owners[chosen]
        inputs = normed[targets]
        gate_part = jnp.dot(inputs, gate_weight[expert], preferred_element_type=jnp.float32)
        up_part = jnp.dot(inputs, up_weight[expert], preferred_element_type=jnp.float32)
        inner_rows = (jax.nn.silu(gate_part) * up_part).astype(jnp.bfloat16)
        pieces = jnp.einsum('mtf,tfd->mtd', inner_rows.reshape(most_rows, N_TP, slice_width).astype(jnp.float32), down_weight[expert].reshape(N_TP, slice_width, D).astype(jnp.float32))
        pieces = lax.optimization_barrier(pieces.astype(jnp.bfloat16)).astype(jnp.float32)
        result = lax.optimization_barrier(lax.optimization_barrier(jnp.sum(pieces, axis=1)).astype(jnp.bfloat16)).astype(jnp.float32)
        scaled = result * (flat_weights[chosen] * filled)[:, None]
        return (gathered.at[targets].add(scaled), None)
    moe_sum, leftover = lax.scan(expert_step, jnp.zeros((LENGTH, D), jnp.float32), jnp.arange(EXPERTS, dtype=jnp.int32))
    return (updated.astype(jnp.float32) + moe_sum).astype(jnp.bfloat16)
```

```python
import functools
import math

import jax
import jax.numpy as jnp
from jax import lax
from jax.experimental import pallas as pl
from jax.experimental.pallas import tpu as pltpu
from jax.sharding import PartitionSpec as P

MESH = pl.DeviceIdType.MESH
LOG2E = 1.4426950408889634
CORES = 2
VMEM_BYTES = 67043328


def attend_kernel(
    n_sp,
    n_tp,
    scale,
    lam_ref,
    q_ref,
    kv_ref,
    gain_ref,
    meta_ref,
    out_ref,
    zmeta_ref,
    kvbuf,
    acc,
    top,
    tot,
    att,
    kv_send,
    kv_recv,
    at_send,
    at_recv,
    me_send,
    me_recv,
    own_sem,
):
    heads, tiles, wide, _ = q_ref.shape
    tile = wide // 2
    rows = out_ref.shape[1]
    n_z = n_tp // CORES
    c = lax.axis_index("sp")
    t = lax.axis_index("tp")
    barrier = pltpu.get_barrier_semaphore()
    for d in range(1, n_sp):
        pl.semaphore_signal(barrier, inc=1, device_id=((c + d) % n_sp, t), device_id_type=MESH)
    for d in range(1, n_tp):
        pl.semaphore_signal(barrier, inc=1, device_id=(c, (t + d) % n_tp), device_id_type=MESH)
    pl.semaphore_wait(barrier, n_sp + n_tp - 2)

    def kv_copy(d, h):
        return pltpu.make_async_remote_copy(
            src_ref=kv_ref.at[h],
            dst_ref=kvbuf.at[d - 1, h],
            send_sem=kv_send.at[d - 1, h],
            recv_sem=kv_recv.at[d - 1, h],
            device_id=((c + d) % n_sp, t),
            device_id_type=MESH,
        )

    def meta_copy(d):
        return pltpu.make_async_remote_copy(
            src_ref=meta_ref,
            dst_ref=zmeta_ref.at[d],
            send_sem=me_send.at[d],
            recv_sem=me_recv.at[d],
            device_id=(c, (t + CORES * d) % n_tp),
            device_id_type=MESH,
        )

    for d in range(1, n_sp):
        @pl.when(c + d < n_sp)
        def _():
            for h in range(heads):
                kv_copy(d, h).start()

    for d in range(1, n_z):
        meta_copy(d).start()
    zmeta_ref[0] = meta_ref[...]

    factor = scale * LOG2E

    def scores_of(h, i, keys):
        return (
            lax.dot_general(
                q_ref[h, i], keys, (((1,), (1,)), ((), ())), preferred_element_type=jnp.float32
            )
            * factor
        )

    for i in range(tiles):
        extent = (i + 1) * tile
        for h in range(heads):
            s = scores_of(h, i, kv_ref[h, 0, :extent])
            row = lax.rem(lax.broadcasted_iota(jnp.int32, (wide, extent), 0), tile) + i * tile
            col = lax.broadcasted_iota(jnp.int32, (wide, extent), 1)
            s = jnp.where(col <= row, s, -jnp.inf)
            high = jnp.max(s, axis=1, keepdims=True)
            p = jnp.exp2(s - high)
            top[h, i] = high
            tot[h, i] = jnp.sum(p, axis=1, keepdims=True)
            acc[h, i] = jnp.dot(
                p.astype(jnp.bfloat16), kv_ref[h, 1, :extent], preferred_element_type=jnp.float32
            )

    def span_step(step, carry):
        for h in range(heads):
            kv_copy(step, h).wait_recv()

        def tile_step(i, inner):
            for h in range(heads):
                s = scores_of(h, i, kvbuf[step - 1, h, 0])
                before = top[h, i]
                high = jnp.maximum(before, jnp.max(s, axis=1, keepdims=True))
                p = jnp.exp2(s - high)
                decay = jnp.exp2(before - high)
                top[h, i] = high
                tot[h, i] = tot[h, i] * decay + jnp.sum(p, axis=1, keepdims=True)
                acc[h, i] = acc[h, i] * decay + jnp.dot(
                    p.astype(jnp.bfloat16),
                    kvbuf[step - 1, h, 1],
                    preferred_element_type=jnp.float32,
                )
            return inner

        return lax.fori_loop(0, tiles, tile_step, carry)

    lax.fori_loop(1, c + 1, span_step, 0)

    for h in range(heads):
        width = acc.shape[3]
        for i in range(tiles):
            both = acc[h, i] / tot[h, i]
            mixed = both[:tile] - lam_ref[h] * both[tile:]
            mean = jnp.mean(mixed * mixed, axis=1, keepdims=True)
            normed = mixed * lax.rsqrt(mean + 1e-06) * gain_ref[...]
            att[i * tile : (i + 1) * tile, h * width : (h + 1) * width] = normed.astype(att.dtype)

    def att_copy(d):
        to = (t + d) % n_tp
        return pltpu.make_async_remote_copy(
            src_ref=att.at[pl.ds(pl.multiple_of(to * rows, rows), rows)],
            dst_ref=out_ref.at[t],
            send_sem=at_send.at[d],
            recv_sem=at_recv.at[d],
            device_id=(c, to),
            device_id_type=MESH,
        )

    for d in range(1, n_tp):
        att_copy(d).start()
    own = pltpu.make_async_copy(
        att.at[pl.ds(pl.multiple_of(t * rows, rows), rows)], out_ref.at[t], own_sem
    )
    own.start()
    own.wait()
    for d in range(1, n_tp):
        att_copy(d).wait()
    for d in range(1, n_z):
        meta_copy(d).wait()
    for d in range(1, n_sp):
        @pl.when(c + d < n_sp)
        def _():
            for h in range(heads):
                kv_copy(d, h).wait_send()


def attend(queries, key_pairs, head_values, lambdas, head_gain, meta, rows, n_sp, n_tp):
    tokens, heads, pair = queries.shape
    width = head_values.shape[2]
    half = pair // 2
    tile = math.gcd(tokens, 256)
    tiles = tokens // tile
    first = (jnp.arange(pair) < half)[None, :]
    q = jnp.transpose(queries, (1, 0, 2)).reshape(heads, tiles, 1, tile, pair)
    sides = jnp.stack([first, ~first])
    q = jnp.where(sides, q, jnp.zeros((), q.dtype)).reshape(heads, tiles, 2 * tile, pair)
    kv = jnp.transpose(jnp.stack([key_pairs, head_values]), (2, 0, 1, 3))
    dma = pltpu.SemaphoreType.DMA
    vmem = pl.BlockSpec(memory_space=pltpu.VMEM)
    n_z = n_tp // CORES
    return pl.pallas_call(
        functools.partial(attend_kernel, n_sp, n_tp, half ** (-0.5)),
        out_shape=(
            jax.ShapeDtypeStruct((n_tp, rows, heads * width), jnp.bfloat16),
            jax.ShapeDtypeStruct((n_z,) + meta.shape, meta.dtype),
        ),
        in_specs=[pl.BlockSpec(memory_space=pltpu.SMEM)] + [vmem] * 4,
        out_specs=(vmem, vmem),
        scratch_shapes=[
            pltpu.VMEM((n_sp - 1,) + kv.shape, kv.dtype),
            pltpu.VMEM((heads, tiles, 2 * tile, width), jnp.float32),
            pltpu.VMEM((heads, tiles, 2 * tile, 1), jnp.float32),
            pltpu.VMEM((heads, tiles, 2 * tile, 1), jnp.float32),
            pltpu.VMEM((tokens, heads * width), jnp.bfloat16),
            dma((n_sp - 1, heads)),
            dma((n_sp - 1, heads)),
            dma((n_tp,)),
            dma((n_tp,)),
            dma((n_z,)),
            dma((n_z,)),
            dma,
        ],
        compiler_params=pltpu.CompilerParams(
            collective_id=0, has_side_effects=True, vmem_limit_bytes=48 * 1024 * 1024
        ),
        name="attend",
    )(lambdas, q, kv, head_gain.reshape(1, -1), meta)


def experts_kernel(
    n_sp,
    n_z,
    x_ref,
    meta_ref,
    base_ref,
    gate_hbm,
    up_hbm,
    down_hbm,
    out_ref,
    gate,
    up,
    down,
    zrows,
    pack,
    arrived,
    psend,
    own,
    precv,
    ret,
    zsend,
    zret,
    w_sem,
    zs_send,
    zs_recv,
    ps_send,
    ps_recv,
    fw_send,
    fw_recv,
    pp_send,
    pp_recv,
    rt_send,
    rt_recv,
    zr_send,
    zr_recv,
):
    rows, model = x_ref.shape
    local, cap = pack.shape[2], pack.shape[3]
    slots = n_sp * local * cap
    c = lax.axis_index("sp")
    t = lax.axis_index("tp")
    n_tp = n_z * CORES
    core = t % CORES
    partner = (c, t + 1 - 2 * core)
    loads = [
        pltpu.make_async_copy(a, b, w_sem.at[i])
        for i, (a, b) in enumerate(((gate_hbm, gate), (up_hbm, up), (down_hbm, down)))
    ]
    for load in loads:
        load.start()

    def column(d):
        return ((c + d) % n_sp, t)

    def layer(d):
        return (c, (t + CORES * d) % n_tp)

    barrier = pltpu.get_barrier_semaphore()
    for d in range(1, n_sp):
        pl.semaphore_signal(barrier, inc=1, device_id=column(d), device_id_type=MESH)
    for d in range(1, n_z):
        pl.semaphore_signal(barrier, inc=1, device_id=layer(d), device_id_type=MESH)
    pl.semaphore_signal(barrier, inc=1, device_id=partner, device_id_type=MESH)
    pl.semaphore_wait(barrier, n_sp + n_z - 1)

    def remote(src, dst, send, recv, target):
        return pltpu.make_async_remote_copy(
            src_ref=src,
            dst_ref=dst,
            send_sem=send,
            recv_sem=recv,
            device_id=target,
            device_id_type=MESH,
        )

    def z_copy(d):
        return remote(x_ref, zrows.at[d - 1], zs_send.at[d], zs_recv.at[d], layer(d))

    def pack_copy(d, s):
        return remote(
            pack.at[d - 1, s], arrived.at[0, d, s], ps_send.at[d, s], ps_recv.at[d, s], column(d)
        )

    def share_copy(d, s):
        return remote(
            arrived.at[0, d, s], arrived.at[1, d, s], fw_send.at[d, s], fw_recv.at[d, s], partner
        )

    def pair_copy(d):
        return remote(psend.at[d], precv.at[d], pp_send.at[d], pp_recv.at[d], partner)

    def back_copy(d):
        return remote(own.at[d], ret.at[d], rt_send.at[d], rt_recv.at[d], column(n_sp - d))

    def z_back(d):
        return remote(
            zsend.at[d], zret.at[d], zr_send.at[d], zr_recv.at[d], layer(n_z - d)
        )

    for d in range(1, n_z):
        z_copy(d).start()

    def route_hits(s, r):
        target = lax.broadcasted_iota(jnp.int32, (slots, rows), 0).astype(jnp.float32)
        return target == meta_ref[s, r : r + 1, :rows]

    for s in range(n_z):
        if s:
            z_copy(s).wait_recv()
        hits = route_hits(s, 0) | route_hits(s, 1)
        pick = jnp.where(hits, 1.0, 0.0).astype(jnp.bfloat16)
        source = x_ref[...] if s == 0 else zrows[s - 1]
        packed = (
            jnp.dot(pick, source, preferred_element_type=jnp.float32)
            .astype(jnp.bfloat16)
            .reshape(n_sp, local, cap, model)
        )
        for d in range(1, n_sp):
            pack[d - 1, s] = packed[d]
            pack_copy(d, s).start()
        arrived[0, 0, s] = packed[0]
        share_copy(0, s).start()

    for load in loads:
        load.wait()

    def reduce_pair(d):
        pair_copy(d).wait_recv()
        total = own[d].astype(jnp.float32) + precv[d].astype(jnp.float32)
        total = total.astype(jnp.bfloat16)
        if d == 0:
            ret[0] = total
        else:
            own[d] = total
            back_copy(d).start()

    for d in range(n_sp):
        if d:
            for s in range(n_z):
                pack_copy(d, s).wait_recv()
                share_copy(d, s).start()
        for s in range(n_z):
            share_copy(d, s).wait_recv()

        def expert_step(e, carry):
            x = arrived[:, d, :, e].reshape(2 * n_z * cap, model)
            gated = jnp.dot(x, gate[e], preferred_element_type=jnp.float32)
            lifted = jnp.dot(x, up[e], preferred_element_type=jnp.float32)
            inner = (gated / (1.0 + jnp.exp(-gated)) * lifted).astype(jnp.bfloat16)
            y = jnp.dot(inner, down[e], preferred_element_type=jnp.float32)
            y = y.astype(jnp.bfloat16).reshape(2, n_z, cap, model)
            own[d, :, e] = y[0]
            psend[d, :, e] = y[1]
            return carry

        lax.fori_loop(0, local, expert_step, 0)
        pair_copy(d).start()
        if d:
            reduce_pair(d - 1)
    reduce_pair(n_sp - 1)
    for d in range(1, n_sp):
        back_copy(d).wait_recv()

    for s in list(range(1, n_z)) + [0]:
        mixing = jnp.where(route_hits(s, 0), meta_ref[s, 2:3, :rows], 0.0) + jnp.where(
            route_hits(s, 1), meta_ref[s, 3:4, :rows], 0.0
        )
        high = mixing.astype(jnp.bfloat16)
        low = (mixing - high.astype(jnp.float32)).astype(jnp.bfloat16)
        back = ret[:, s].reshape(slots, model)
        numbers = (((0,), (0,)), ((), ()))
        merged = lax.dot_general(
            high, back, numbers, preferred_element_type=jnp.float32
        ) + lax.dot_general(low, back, numbers, preferred_element_type=jnp.float32)
        if s:
            zsend[s] = merged.astype(jnp.bfloat16)
            z_back(s).start()
    for s in range(1, n_z):
        z_back(s).wait_recv()
        merged = merged + zret[s].astype(jnp.float32)
    out_ref[...] = (base_ref[...].astype(jnp.float32) + merged).astype(jnp.bfloat16)

    for d in range(1, n_z):
        z_copy(d).wait_send()
        z_back(d).wait_send()
    for d in range(n_sp):
        for s in range(n_z):
            if d:
                pack_copy(d, s).wait_send()
            share_copy(d, s).wait_send()
        pair_copy(d).wait_send()
        if d:
            back_copy(d).wait_send()


def experts(normed, zmeta, updated, gate_weight, up_weight, down_weight, n_sp, n_z, cap):
    rows, model = normed.shape
    local = gate_weight.shape[0]
    dma = pltpu.SemaphoreType.DMA
    vmem = pl.BlockSpec(memory_space=pltpu.VMEM)
    hbm = pl.BlockSpec(memory_space=pl.ANY)
    block = (n_z, local, cap, model)

    def buffer(*shape):
        return pltpu.VMEM(shape, jnp.bfloat16)

    return pl.pallas_call(
        functools.partial(experts_kernel, n_sp, n_z),
        out_shape=jax.ShapeDtypeStruct((rows, model), jnp.bfloat16),
        in_specs=[vmem] * 3 + [hbm] * 3,
        out_specs=vmem,
        scratch_shapes=[
            buffer(*gate_weight.shape),
            buffer(*up_weight.shape),
            buffer(*down_weight.shape),
            buffer(n_z - 1, rows, model),
            buffer(n_sp - 1, *block),
            buffer(2, n_sp, *block),
            buffer(n_sp, *block),
            buffer(n_sp, *block),
            buffer(n_sp, *block),
            buffer(n_sp, *block),
            buffer(n_z, rows, model),
            buffer(n_z, rows, model),
            dma((3,)),
            dma((n_z,)),
            dma((n_z,)),
            dma((n_sp, n_z)),
            dma((n_sp, n_z)),
            dma((n_sp, n_z)),
            dma((n_sp, n_z)),
            dma((n_sp,)),
            dma((n_sp,)),
            dma((n_sp,)),
            dma((n_sp,)),
            dma((n_z,)),
            dma((n_z,)),
        ],
        compiler_params=pltpu.CompilerParams(
            collective_id=1, has_side_effects=True, vmem_limit_bytes=VMEM_BYTES
        ),
        name="experts",
    )(normed, zmeta, updated, gate_weight, up_weight, down_weight)


def shards(
    queries,
    key_pairs,
    head_values,
    lambdas,
    head_gain,
    out_weight,
    residual,
    norm_gain,
    expert_ids,
    route_weights,
    gate_weight,
    up_weight,
    down_weight,
):
    tokens_here, heads_here, pair_width = queries.shape
    value_width = head_values.shape[2]
    rows_here = residual.shape[0]
    sp_count = lax.axis_size("sp")
    tp_count = lax.axis_size("tp")
    z_count = tp_count // CORES
    route_count = expert_ids.shape[1]
    local_experts = gate_weight.shape[0]
    expert_count = local_experts * sp_count
    capacity = max(2, 4 * rows_here * route_count // (3 * expert_count))
    flat_ids = expert_ids.reshape(-1)
    indicator = (flat_ids[:, None] == jnp.arange(expert_count, dtype=jnp.int32)[None, :]).astype(
        jnp.int32
    )
    ranking = jnp.sum(jnp.cumsum(indicator, axis=0) * indicator, axis=1) - 1
    turned = (flat_ids - lax.axis_index("sp") * local_experts) % expert_count
    near_slots = (turned * capacity + ranking).reshape(rows_here, route_count)
    slots = flat_ids * capacity + ranking
    meta = jnp.concatenate([near_slots.astype(jnp.float32), route_weights], axis=1).T
    meta = jnp.pad(meta, ((0, 8 - 2 * route_count), (0, -rows_here % 128)), constant_values=-1.0)
    gathered, zmeta = attend(
        queries, key_pairs, head_values, lambdas, head_gain, meta, rows_here, sp_count, tp_count
    )
    regrouped = jnp.transpose(gathered, (1, 0, 2)).reshape(rows_here, -1)
    projected = jnp.dot(regrouped, out_weight, preferred_element_type=jnp.float32)
    updated = (residual.astype(jnp.float32) + projected).astype(jnp.bfloat16)
    widened = updated.astype(jnp.float32)
    normed = (
        widened * lax.rsqrt(jnp.mean(widened * widened, axis=1, keepdims=True) + 1e-06) * norm_gain
    ).astype(jnp.bfloat16)
    model_width = normed.shape[1]
    block_bytes = z_count * local_experts * capacity * model_width * 2
    if capacity % 16 == 0 and rows_here <= 128 and route_count == 2 and (
        (7 * sp_count - 1) * block_bytes <= 3 * VMEM_BYTES // 5
    ):
        return experts(
            normed, zmeta, updated, gate_weight, up_weight, down_weight, sp_count, z_count, capacity
        )
    sources = jnp.arange(rows_here * route_count, dtype=jnp.int32) // route_count
    outgoing = (
        jnp.zeros((expert_count * capacity, model_width), jnp.bfloat16)
        .at[slots]
        .set(normed[sources])
    )
    arrived = lax.all_to_all(
        outgoing.reshape(sp_count, local_experts, capacity, model_width),
        "sp",
        split_axis=0,
        concat_axis=0,
        tiled=True,
    )
    piece_rows = lax.all_gather(arrived[None], "tp", axis=0, tiled=True)
    gate_part = jnp.einsum(
        "tsecd,edf->tsecf", piece_rows, gate_weight, preferred_element_type=jnp.float32
    )
    up_part = jnp.einsum(
        "tsecd,edf->tsecf", piece_rows, up_weight, preferred_element_type=jnp.float32
    )
    inner_rows = (jax.nn.silu(gate_part) * up_part).astype(jnp.bfloat16)
    partial_value = jnp.einsum(
        "tsecf,efd->tsecd", inner_rows, down_weight, preferred_element_type=jnp.float32
    )
    reduced = lax.psum_scatter(
        partial_value.astype(jnp.bfloat16), "tp", scatter_dimension=0, tiled=True
    )
    returned = lax.all_to_all(reduced[0], "sp", split_axis=0, concat_axis=0, tiled=True)
    picked = (
        returned.reshape(expert_count * capacity, model_width)[slots]
        .astype(jnp.float32)
        .reshape(rows_here, route_count, model_width)
    )
    moe_sum = jnp.sum(picked * route_weights[:, :, None], axis=1)
    return (updated.astype(jnp.float32) + moe_sum).astype(jnp.bfloat16)


def solution(mesh):
    placed = (
        P("sp", "tp", None),
        P("sp", "tp", None),
        P("sp", "tp", None),
        P("tp"),
        P(),
        P(),
        P(("sp", "tp"), None),
        P(),
        P(("sp", "tp"), None),
        P(("sp", "tp"), None),
        P("sp", None, "tp"),
        P("sp", None, "tp"),
        P("sp", "tp", None),
    )
    return jax.shard_map(
        shards, mesh=mesh, in_specs=placed, out_specs=P(("sp", "tp"), None), check_vma=False
    )
```

```python
import functools
import math

import jax
import jax.numpy as jnp
from jax import lax
from jax.experimental import pallas as pl
from jax.experimental.pallas import tpu as pltpu
from jax.sharding import PartitionSpec as P

MESH = pl.DeviceIdType.MESH
LOG2E = 1.4426950408889634
CORES = 2
VMEM_BYTES = 67043328


def attend_kernel(
    n_sp,
    n_tp,
    scale,
    lam_ref,
    q_ref,
    kv_ref,
    gain_ref,
    meta_ref,
    base_ref,
    norm_ref,
    w_hbm,
    updated_ref,
    normed_ref,
    zmeta_ref,
    weight,
    gathered,
    kvbuf,
    acc,
    top,
    tot,
    att,
    kv_send,
    kv_recv,
    at_send,
    at_recv,
    me_send,
    me_recv,
    own_sem,
    w_sem,
):
    heads, tiles, wide, _ = q_ref.shape
    tile = wide // 2
    rows = base_ref.shape[0]
    n_z = n_tp // CORES
    c = lax.axis_index("sp")
    t = lax.axis_index("tp")
    load = pltpu.make_async_copy(w_hbm, weight, w_sem)
    load.start()
    barrier = pltpu.get_barrier_semaphore()
    for d in range(1, n_sp):
        pl.semaphore_signal(barrier, inc=1, device_id=((c + d) % n_sp, t), device_id_type=MESH)
    for d in range(1, n_tp):
        pl.semaphore_signal(barrier, inc=1, device_id=(c, (t + d) % n_tp), device_id_type=MESH)
    pl.semaphore_wait(barrier, n_sp + n_tp - 2)

    def kv_copy(d, h):
        return pltpu.make_async_remote_copy(
            src_ref=kv_ref.at[h],
            dst_ref=kvbuf.at[d - 1, h],
            send_sem=kv_send.at[d - 1, h],
            recv_sem=kv_recv.at[d - 1, h],
            device_id=((c + d) % n_sp, t),
            device_id_type=MESH,
        )

    def meta_copy(d):
        return pltpu.make_async_remote_copy(
            src_ref=meta_ref,
            dst_ref=zmeta_ref.at[d],
            send_sem=me_send.at[d],
            recv_sem=me_recv.at[d],
            device_id=(c, (t + CORES * d) % n_tp),
            device_id_type=MESH,
        )

    for d in range(1, n_sp):
        @pl.when(c + d < n_sp)
        def _():
            for h in range(heads):
                kv_copy(d, h).start()

    for d in range(1, n_z):
        meta_copy(d).start()
    zmeta_ref[0] = meta_ref[...]

    factor = scale * LOG2E

    def scores_of(h, i, keys):
        return (
            lax.dot_general(
                q_ref[h, i], keys, (((1,), (1,)), ((), ())), preferred_element_type=jnp.float32
            )
            * factor
        )

    for i in range(tiles):
        extent = (i + 1) * tile
        for h in range(heads):
            s = scores_of(h, i, kv_ref[h, 0, :extent])
            row = lax.rem(lax.broadcasted_iota(jnp.int32, (wide, extent), 0), tile) + i * tile
            col = lax.broadcasted_iota(jnp.int32, (wide, extent), 1)
            s = jnp.where(col <= row, s, -jnp.inf)
            high = jnp.max(s, axis=1, keepdims=True)
            p = jnp.exp2(s - high)
            top[h, i] = high
            tot[h, i] = jnp.sum(p, axis=1, keepdims=True)
            acc[h, i] = jnp.dot(
                p.astype(jnp.bfloat16), kv_ref[h, 1, :extent], preferred_element_type=jnp.float32
            )

    def span_step(step, carry):
        for h in range(heads):
            kv_copy(step, h).wait_recv()

        def tile_step(i, inner):
            for h in range(heads):
                s = scores_of(h, i, kvbuf[step - 1, h, 0])
                before = top[h, i]
                high = jnp.maximum(before, jnp.max(s, axis=1, keepdims=True))
                p = jnp.exp2(s - high)
                decay = jnp.exp2(before - high)
                top[h, i] = high
                tot[h, i] = tot[h, i] * decay + jnp.sum(p, axis=1, keepdims=True)
                acc[h, i] = acc[h, i] * decay + jnp.dot(
                    p.astype(jnp.bfloat16),
                    kvbuf[step - 1, h, 1],
                    preferred_element_type=jnp.float32,
                )
            return inner

        return lax.fori_loop(0, tiles, tile_step, carry)

    lax.fori_loop(1, c + 1, span_step, 0)

    for h in range(heads):
        width = acc.shape[3]
        for i in range(tiles):
            both = acc[h, i] / tot[h, i]
            mixed = both[:tile] - lam_ref[h] * both[tile:]
            mean = jnp.mean(mixed * mixed, axis=1, keepdims=True)
            normed = mixed * lax.rsqrt(mean + 1e-06) * gain_ref[...]
            att[i * tile : (i + 1) * tile, h * width : (h + 1) * width] = normed.astype(att.dtype)

    def att_copy(d):
        to = (t + d) % n_tp
        return pltpu.make_async_remote_copy(
            src_ref=att.at[pl.ds(pl.multiple_of(to * rows, rows), rows)],
            dst_ref=gathered.at[t],
            send_sem=at_send.at[d],
            recv_sem=at_recv.at[d],
            device_id=(c, to),
            device_id_type=MESH,
        )

    for d in range(1, n_tp):
        att_copy(d).start()
    own = pltpu.make_async_copy(
        att.at[pl.ds(pl.multiple_of(t * rows, rows), rows)], gathered.at[t], own_sem
    )
    own.start()
    own.wait()
    load.wait()
    span = att.shape[1]
    projected = jnp.zeros(base_ref.shape, jnp.float32)
    for d in range(n_tp):
        if d:
            att_copy(d).wait_recv()
        source = (t - d + n_tp) % n_tp
        projected = projected + jnp.dot(
            gathered[source],
            weight[pl.ds(pl.multiple_of(source * span, span), span), :],
            preferred_element_type=jnp.float32,
        )
    updated = (base_ref[...].astype(jnp.float32) + projected).astype(jnp.bfloat16)
    updated_ref[...] = updated
    widened = updated.astype(jnp.float32)
    mean = jnp.mean(widened * widened, axis=1, keepdims=True)
    normed_ref[...] = (widened * lax.rsqrt(mean + 1e-06) * norm_ref[...]).astype(jnp.bfloat16)
    for d in range(1, n_tp):
        att_copy(d).wait_send()
    for d in range(1, n_z):
        meta_copy(d).wait()
    for d in range(1, n_sp):
        @pl.when(c + d < n_sp)
        def _():
            for h in range(heads):
                kv_copy(d, h).wait_send()


def attend(queries, key_pairs, head_values, lambdas, head_gain, meta, residual, norm_gain, out_weight, n_sp, n_tp):
    tokens, heads, pair = queries.shape
    rows = residual.shape[0]
    width = head_values.shape[2]
    half = pair // 2
    tile = math.gcd(tokens, 256)
    tiles = tokens // tile
    first = (jnp.arange(pair) < half)[None, :]
    q = jnp.transpose(queries, (1, 0, 2)).reshape(heads, tiles, 1, tile, pair)
    sides = jnp.stack([first, ~first])
    q = jnp.where(sides, q, jnp.zeros((), q.dtype)).reshape(heads, tiles, 2 * tile, pair)
    kv = jnp.transpose(jnp.stack([key_pairs, head_values]), (2, 0, 1, 3))
    dma = pltpu.SemaphoreType.DMA
    vmem = pl.BlockSpec(memory_space=pltpu.VMEM)
    n_z = n_tp // CORES
    return pl.pallas_call(
        functools.partial(attend_kernel, n_sp, n_tp, half ** (-0.5)),
        out_shape=(
            jax.ShapeDtypeStruct(residual.shape, jnp.bfloat16),
            jax.ShapeDtypeStruct(residual.shape, jnp.bfloat16),
            jax.ShapeDtypeStruct((n_z,) + meta.shape, meta.dtype),
        ),
        in_specs=[pl.BlockSpec(memory_space=pltpu.SMEM)] + [vmem] * 6
        + [pl.BlockSpec(memory_space=pl.ANY)],
        out_specs=(vmem, vmem, vmem),
        scratch_shapes=[
            pltpu.VMEM(out_weight.shape, out_weight.dtype),
            pltpu.VMEM((n_tp, rows, heads * width), jnp.bfloat16),
            pltpu.VMEM((n_sp - 1,) + kv.shape, kv.dtype),
            pltpu.VMEM((heads, tiles, 2 * tile, width), jnp.float32),
            pltpu.VMEM((heads, tiles, 2 * tile, 1), jnp.float32),
            pltpu.VMEM((heads, tiles, 2 * tile, 1), jnp.float32),
            pltpu.VMEM((tokens, heads * width), jnp.bfloat16),
            dma((n_sp - 1, heads)),
            dma((n_sp - 1, heads)),
            dma((n_tp,)),
            dma((n_tp,)),
            dma((n_z,)),
            dma((n_z,)),
            dma,
            dma,
        ],
        compiler_params=pltpu.CompilerParams(
            collective_id=0, has_side_effects=True, vmem_limit_bytes=48 * 1024 * 1024
        ),
        name="attend",
    )(lambdas, q, kv, head_gain.reshape(1, -1), meta, residual, norm_gain.reshape(1, -1), out_weight)


def experts_kernel(
    n_sp,
    n_z,
    x_ref,
    meta_ref,
    base_ref,
    gate_hbm,
    up_hbm,
    down_hbm,
    out_ref,
    gate,
    up,
    down,
    zrows,
    pack,
    arrived,
    psend,
    own,
    precv,
    ret,
    zsend,
    zret,
    mine,
    w_sem,
    zs_send,
    zs_recv,
    ps_send,
    ps_recv,
    fw_send,
    fw_recv,
    pp_send,
    pp_recv,
    rt_send,
    rt_recv,
    zr_send,
    zr_recv,
):
    rows, model = x_ref.shape
    local, cap = pack.shape[2], pack.shape[3]
    slots = n_sp * local * cap
    c = lax.axis_index("sp")
    t = lax.axis_index("tp")
    n_tp = n_z * CORES
    core = t % CORES
    partner = (c, t + 1 - 2 * core)
    loads = [
        pltpu.make_async_copy(a, b, w_sem.at[i])
        for i, (a, b) in enumerate(((gate_hbm, gate), (up_hbm, up), (down_hbm, down)))
    ]
    for load in loads:
        load.start()

    def column(d):
        return ((c + d) % n_sp, t)

    def layer(d):
        return (c, (t + CORES * d) % n_tp)

    barrier = pltpu.get_barrier_semaphore()
    for d in range(1, n_sp):
        pl.semaphore_signal(barrier, inc=1, device_id=column(d), device_id_type=MESH)
    for d in range(1, n_z):
        pl.semaphore_signal(barrier, inc=1, device_id=layer(d), device_id_type=MESH)
    pl.semaphore_signal(barrier, inc=1, device_id=partner, device_id_type=MESH)
    pl.semaphore_wait(barrier, n_sp + n_z - 1)

    def remote(src, dst, send, recv, target):
        return pltpu.make_async_remote_copy(
            src_ref=src,
            dst_ref=dst,
            send_sem=send,
            recv_sem=recv,
            device_id=target,
            device_id_type=MESH,
        )

    def z_copy(d):
        return remote(x_ref, zrows.at[d - 1], zs_send.at[d], zs_recv.at[d], layer(d))

    def pack_copy(d, s):
        return remote(
            pack.at[s, d - 1], arrived.at[0, s, d], ps_send.at[d, s], ps_recv.at[d, s], column(d)
        )

    def share_copy(d, s):
        return remote(
            arrived.at[0, s, d], arrived.at[1, s, d], fw_send.at[d, s], fw_recv.at[d, s], partner
        )

    def pair_copy(s):
        return remote(psend.at[s], precv.at[s], pp_send.at[s], pp_recv.at[s], partner)

    def back_copy(d, s):
        return remote(
            own.at[s, d], ret.at[s, d], rt_send.at[d, s], rt_recv.at[d, s], column(n_sp - d)
        )

    def z_back(d):
        return remote(
            zsend.at[d], zret.at[d], zr_send.at[d], zr_recv.at[d], layer(n_z - d)
        )

    for d in range(1, n_z):
        z_copy(d).start()

    def route_hits(s, r):
        target = lax.broadcasted_iota(jnp.int32, (slots, rows), 0).astype(jnp.float32)
        return target == meta_ref[s, r : r + 1, :rows]

    def pack_rows(s):
        if s:
            z_copy(s).wait_recv()
        hits = route_hits(s, 0) | route_hits(s, 1)
        pick = jnp.where(hits, 1.0, 0.0).astype(jnp.bfloat16)
        source = x_ref[...] if s == 0 else zrows[s - 1]
        packed = (
            jnp.dot(pick, source, preferred_element_type=jnp.float32)
            .astype(jnp.bfloat16)
            .reshape(n_sp, local, cap, model)
        )
        for d in range(1, n_sp):
            pack[s, d - 1] = packed[d]
            pack_copy(d, s).start()
        arrived[0, s, 0] = packed[0]
        share_copy(0, s).start()

    def run_experts(s):
        for d in range(1, n_sp):
            pack_copy(d, s).wait_recv()
            share_copy(d, s).start()
        for d in range(n_sp):
            share_copy(d, s).wait_recv()

        def expert_step(e, carry):
            x = arrived[:, s, :, e].reshape(2 * n_sp * cap, model)
            gated = jnp.dot(x, gate[e], preferred_element_type=jnp.float32)
            lifted = jnp.dot(x, up[e], preferred_element_type=jnp.float32)
            inner = (gated / (1.0 + jnp.exp(-gated)) * lifted).astype(jnp.bfloat16)
            y = jnp.dot(inner, down[e], preferred_element_type=jnp.float32)
            y = y.astype(jnp.bfloat16).reshape(2, n_sp, cap, model)
            own[s, :, e] = y[0]
            psend[s, :, e] = y[1]
            return carry

        lax.fori_loop(0, local, expert_step, 0)
        pair_copy(s).start()

    def reduce_pair(s):
        pair_copy(s).wait_recv()
        for d in list(range(1, n_sp)) + [0]:
            total = own[s, d].astype(jnp.float32) + precv[s, d].astype(jnp.float32)
            total = total.astype(jnp.bfloat16)
            if d == 0:
                ret[s, 0] = total
            else:
                own[s, d] = total
                back_copy(d, s).start()

    def mix_rows(s):
        for d in range(1, n_sp):
            back_copy(d, s).wait_recv()
        mixing = jnp.where(route_hits(s, 0), meta_ref[s, 2:3, :rows], 0.0) + jnp.where(
            route_hits(s, 1), meta_ref[s, 3:4, :rows], 0.0
        )
        high = mixing.astype(jnp.bfloat16)
        low = (mixing - high.astype(jnp.float32)).astype(jnp.bfloat16)
        back = ret[s].reshape(slots, model)
        numbers = (((0,), (0,)), ((), ()))
        merged = lax.dot_general(
            high, back, numbers, preferred_element_type=jnp.float32
        ) + lax.dot_general(low, back, numbers, preferred_element_type=jnp.float32)
        if s:
            zsend[s] = merged.astype(jnp.bfloat16)
            z_back(s).start()
        else:
            mine[...] = merged

    pack_rows(0)
    for load in loads:
        load.wait()
    if n_z > 1:
        pack_rows(1)
    for s in range(n_z):
        run_experts(s)
        if s + 2 < n_z:
            pack_rows(s + 2)
        elif s + 2 - n_z < n_z - 2:
            mix_rows(s + 2 - n_z)
        reduce_pair(s)
    for s in range(max(0, n_z - 2), n_z):
        mix_rows(s)
    merged = mine[...]
    for s in range(1, n_z):
        z_back(s).wait_recv()
        merged = merged + zret[s].astype(jnp.float32)
    out_ref[...] = (base_ref[...].astype(jnp.float32) + merged).astype(jnp.bfloat16)

    for d in range(1, n_z):
        z_copy(d).wait_send()
        z_back(d).wait_send()
    for s in range(n_z):
        for d in range(n_sp):
            if d:
                pack_copy(d, s).wait_send()
                back_copy(d, s).wait_send()
            share_copy(d, s).wait_send()
        pair_copy(s).wait_send()


def experts(normed, zmeta, updated, gate_weight, up_weight, down_weight, n_sp, n_z, cap):
    rows, model = normed.shape
    local = gate_weight.shape[0]
    dma = pltpu.SemaphoreType.DMA
    vmem = pl.BlockSpec(memory_space=pltpu.VMEM)
    hbm = pl.BlockSpec(memory_space=pl.ANY)
    block = (local, cap, model)

    def buffer(*shape):
        return pltpu.VMEM(shape, jnp.bfloat16)

    return pl.pallas_call(
        functools.partial(experts_kernel, n_sp, n_z),
        out_shape=jax.ShapeDtypeStruct((rows, model), jnp.bfloat16),
        in_specs=[vmem] * 3 + [hbm] * 3,
        out_specs=vmem,
        scratch_shapes=[
            buffer(*gate_weight.shape),
            buffer(*up_weight.shape),
            buffer(*down_weight.shape),
            buffer(n_z - 1, rows, model),
            buffer(n_z, n_sp - 1, *block),
            buffer(2, n_z, n_sp, *block),
            buffer(n_z, n_sp, *block),
            buffer(n_z, n_sp, *block),
            buffer(n_z, n_sp, *block),
            buffer(n_z, n_sp, *block),
            buffer(n_z, rows, model),
            buffer(n_z, rows, model),
            pltpu.VMEM((rows, model), jnp.float32),
            dma((3,)),
            dma((n_z,)),
            dma((n_z,)),
            dma((n_sp, n_z)),
            dma((n_sp, n_z)),
            dma((n_sp, n_z)),
            dma((n_sp, n_z)),
            dma((n_z,)),
            dma((n_z,)),
            dma((n_sp, n_z)),
            dma((n_sp, n_z)),
            dma((n_z,)),
            dma((n_z,)),
        ],
        compiler_params=pltpu.CompilerParams(
            collective_id=1, has_side_effects=True, vmem_limit_bytes=VMEM_BYTES
        ),
        name="experts",
    )(normed, zmeta, updated, gate_weight, up_weight, down_weight)


def shards(
    queries,
    key_pairs,
    head_values,
    lambdas,
    head_gain,
    out_weight,
    residual,
    norm_gain,
    expert_ids,
    route_weights,
    gate_weight,
    up_weight,
    down_weight,
):
    tokens_here, heads_here, pair_width = queries.shape
    value_width = head_values.shape[2]
    rows_here = residual.shape[0]
    sp_count = lax.axis_size("sp")
    tp_count = lax.axis_size("tp")
    z_count = tp_count // CORES
    route_count = expert_ids.shape[1]
    local_experts = gate_weight.shape[0]
    expert_count = local_experts * sp_count
    capacity = max(2, 4 * rows_here * route_count // (3 * expert_count))
    flat_ids = expert_ids.reshape(-1)
    indicator = (flat_ids[:, None] == jnp.arange(expert_count, dtype=jnp.int32)[None, :]).astype(
        jnp.int32
    )
    ranking = jnp.sum(jnp.cumsum(indicator, axis=0) * indicator, axis=1) - 1
    turned = (flat_ids - lax.axis_index("sp") * local_experts) % expert_count
    near_slots = (turned * capacity + ranking).reshape(rows_here, route_count)
    slots = flat_ids * capacity + ranking
    meta = jnp.concatenate([near_slots.astype(jnp.float32), route_weights], axis=1).T
    meta = jnp.pad(meta, ((0, 8 - 2 * route_count), (0, -rows_here % 128)), constant_values=-1.0)
    updated, normed, zmeta = attend(
        queries,
        key_pairs,
        head_values,
        lambdas,
        head_gain,
        meta,
        residual,
        norm_gain,
        out_weight,
        sp_count,
        tp_count,
    )
    model_width = normed.shape[1]
    block_bytes = z_count * local_experts * capacity * model_width * 2
    if capacity % 16 == 0 and rows_here <= 128 and route_count == 2 and (
        (7 * sp_count - 1) * block_bytes <= 3 * VMEM_BYTES // 5
    ):
        return experts(
            normed, zmeta, updated, gate_weight, up_weight, down_weight, sp_count, z_count, capacity
        )
    sources = jnp.arange(rows_here * route_count, dtype=jnp.int32) // route_count
    outgoing = (
        jnp.zeros((expert_count * capacity, model_width), jnp.bfloat16)
        .at[slots]
        .set(normed[sources])
    )
    arrived = lax.all_to_all(
        outgoing.reshape(sp_count, local_experts, capacity, model_width),
        "sp",
        split_axis=0,
        concat_axis=0,
        tiled=True,
    )
    piece_rows = lax.all_gather(arrived[None], "tp", axis=0, tiled=True)
    gate_part = jnp.einsum(
        "tsecd,edf->tsecf", piece_rows, gate_weight, preferred_element_type=jnp.float32
    )
    up_part = jnp.einsum(
        "tsecd,edf->tsecf", piece_rows, up_weight, preferred_element_type=jnp.float32
    )
    inner_rows = (jax.nn.silu(gate_part) * up_part).astype(jnp.bfloat16)
    partial_value = jnp.einsum(
        "tsecf,efd->tsecd", inner_rows, down_weight, preferred_element_type=jnp.float32
    )
    reduced = lax.psum_scatter(
        partial_value.astype(jnp.bfloat16), "tp", scatter_dimension=0, tiled=True
    )
    returned = lax.all_to_all(reduced[0], "sp", split_axis=0, concat_axis=0, tiled=True)
    picked = (
        returned.reshape(expert_count * capacity, model_width)[slots]
        .astype(jnp.float32)
        .reshape(rows_here, route_count, model_width)
    )
    moe_sum = jnp.sum(picked * route_weights[:, :, None], axis=1)
    return (updated.astype(jnp.float32) + moe_sum).astype(jnp.bfloat16)


def solution(mesh):
    placed = (
        P("sp", "tp", None),
        P("sp", "tp", None),
        P("sp", "tp", None),
        P("tp"),
        P(),
        P(),
        P(("sp", "tp"), None),
        P(),
        P(("sp", "tp"), None),
        P(("sp", "tp"), None),
        P("sp", None, "tp"),
        P("sp", None, "tp"),
        P("sp", "tp", None),
    )
    return jax.shard_map(
        shards, mesh=mesh, in_specs=placed, out_specs=P(("sp", "tp"), None), check_vma=False
    )
```
